32 devices in a mesh: row: 8 (over z, x), col: 4 (over y, core).
Axes of the slice: x: 2, y: 2, z: 4, core: 2. Of those that a mesh axis runs over, the one named last changes fastest.
Arguments:
- tokens: bfloat16 [9216, 4096], P('row'), may hold values from -6 to 6
- proj_in: bfloat16 [4096, 512], P(None, 'col'), may hold values from -0.09375 to 0.09375
- proj_out: bfloat16 [512, 4096], P(None, 'col'), may hold values from -0.25 to 0.25
Outputs:
- mixed: bfloat16 [9216, 4096], P('row', 'col')
The draws below stay inside these ranges and needn't reach their ends.
All inputs are finite; a program needn't handle non-finite values.
Results may differ from the reference program's by a relative error of at most 0.0057.
Values may be sent and summed in bfloat16 or wider, within the bound.
No kernel may reach another device: no remote copies, remote signals or barrier semaphores. Data moves between devices by JAX's collectives and lax.ppermute only.
A program may use at most 64 MiB of HBM per device.

```python
import jax
import jax.numpy as jnp

D = 4096
GW = 128
SEQ = 9216
FW = 512
N_COL = 4


def levels(key, dims, cuts, low, high):
    factor_of, own = 1.0, jax.random.fold_in(key, 6)
    for position, parts in cuts:
        steps = jnp.exp(jax.random.uniform(jax.random.fold_in(own, position), (parts,), jnp.float32, low / len(cuts), high / len(cuts)))
        factor_of = factor_of * jnp.repeat(steps, dims[position] // parts).reshape([-1 if axis == position else 1 for axis in range(len(dims))])
    return factor_of


def centred(rng, dims, width, limit, pieces=(), kind=jnp.bfloat16):
    gain = levels(rng, dims, pieces, -0.22, 0.18) if pieces else 1.0
    result = jax.random.normal(rng, dims, jnp.float32) * width * gain
    return jnp.minimum(jnp.maximum(result, -limit), limit).astype(kind)


def setup_inputs(seed: int = 0) -> dict:
    key_of = jax.random.split(jax.random.key(seed), 4)
    tokens = centred(key_of[0], (SEQ, D), 1.0, 6.0, ((0, 8),))
    proj_in = centred(key_of[1], (D, FW), D ** -0.5, 0.09375, ((1, 4),))
    proj_out = centred(key_of[2], (FW, D), FW ** -0.5, 0.25, ((1, 4),))
    return dict(tokens=tokens, proj_in=proj_in, proj_out=proj_out)


def reference(tokens, proj_in, proj_out):
    branch_in = jnp.dot(tokens, proj_in, preferred_element_type=jnp.float32).astype(jnp.bfloat16)
    grouped = branch_in.astype(jnp.float32).reshape(SEQ, N_COL, GW)
    spectrum = jnp.fft.fft2(grouped, axes=(0, 2), norm="ortho").real
    spectrum = spectrum.astype(jnp.bfloat16).reshape(SEQ, FW)
    return jnp.dot(spectrum, proj_out, preferred_element_type=jnp.float32).astype(jnp.bfloat16)
```

```python
import math

import jax
import jax.numpy as jnp
import numpy as np
from jax import lax
from jax.experimental import pallas as pl
from jax.experimental.pallas import tpu as pltpu
from jax.sharding import Mesh, PartitionSpec as P

LANES = 128
ROW = "row"
COL = ("far", "near")


def cos_sin(row_ids, col_ids, period):
    phase_idx = row_ids * col_ids % period
    angles = phase_idx.astype(jnp.float32) * (2.0 * math.pi / period)
    return (jnp.cos(angles), jnp.sin(angles))


def apply_table(form, table_cos, table_sin, real_part, imag_part):
    highest = lax.Precision.HIGHEST
    out_real = jnp.einsum(form, table_cos, real_part, precision=highest) + jnp.einsum(
        form, table_sin, imag_part, precision=highest
    )
    out_imag = jnp.einsum(form, table_cos, imag_part, precision=highest) - jnp.einsum(
        form, table_sin, real_part, precision=highest
    )
    return (out_real, out_imag)


def general_device(tokens, proj_in, proj_out):
    row_count = lax.axis_size(ROW)
    local_rows = tokens.shape[0]
    group_width = proj_in.shape[1]
    seq_length = local_rows * row_count
    row_rank = lax.axis_index(ROW)
    highest = lax.Precision.HIGHEST
    first_len = 16
    second_len = local_rows // first_len
    branch_in = jnp.dot(tokens, proj_in, preferred_element_type=jnp.float32).astype(jnp.bfloat16)
    outer_idx = jnp.arange(row_count, dtype=jnp.int32)
    outer_cos, outer_sin = cos_sin(outer_idx[:, None], outer_idx[None, :], row_count)
    values = lax.all_to_all(
        branch_in.reshape(1, local_rows, group_width),
        "row",
        split_axis=1,
        concat_axis=0,
        tiled=True,
    ).astype(jnp.float32)
    real_part = jnp.einsum("kn,nmg->kmg", outer_cos, values, precision=highest)
    imag_part = -jnp.einsum("kn,nmg->kmg", outer_sin, values, precision=highest)
    real_parts = real_part
    imag_parts = imag_part
    inner_idx = jnp.arange(local_rows, dtype=jnp.int32)
    first_idx = jnp.arange(first_len, dtype=jnp.int32)
    second_idx = jnp.arange(second_len, dtype=jnp.int32)
    first_cos, first_sin = cos_sin(first_idx[:, None], first_idx[None, :], first_len)
    second_cos, second_sin = cos_sin(second_idx[:, None], second_idx[None, :], second_len)
    mid_cos, mid_sin = cos_sin(first_idx[:, None], second_idx[None, :], local_rows)
    mid_cos = mid_cos[None, :, :, None]
    mid_sin = mid_sin[None, :, :, None]
    twid_cos, twid_sin = cos_sin(row_rank, inner_idx, seq_length)
    twid_cos = twid_cos[None, :, None]
    twid_sin = twid_sin[None, :, None]
    real_part = lax.all_to_all(real_parts, "row", split_axis=0, concat_axis=1, tiled=True)
    imag_part = lax.all_to_all(imag_parts, "row", split_axis=0, concat_axis=1, tiled=True)
    real_part, imag_part = (
        real_part * twid_cos + imag_part * twid_sin,
        imag_part * twid_cos - real_part * twid_sin,
    )
    leading = real_part.shape[0]
    items = real_part.shape[2]
    real_part = real_part.reshape(leading, first_len, second_len, items)
    imag_part = imag_part.reshape(leading, first_len, second_len, items)
    real_part, imag_part = apply_table("kn,anqg->akqg", first_cos, first_sin, real_part, imag_part)
    real_part, imag_part = (
        real_part * mid_cos + imag_part * mid_sin,
        imag_part * mid_cos - real_part * mid_sin,
    )
    real_part, imag_part = apply_table(
        "kq,apqg->akpg", second_cos, second_sin, real_part, imag_part
    )
    spec_real = real_part.reshape(leading, local_rows, items)
    spec_imag = imag_part.reshape(leading, local_rows, items)
    channel = jnp.arange(group_width, dtype=jnp.int32)
    chan_cos, chan_sin = cos_sin(channel[:, None], channel[None, :], group_width)
    norm_scale = 1.0 / math.sqrt(seq_length * group_width)
    mixed_real = (
        jnp.dot(
            spec_real.reshape(local_rows, group_width),
            chan_cos,
            precision=highest,
            preferred_element_type=jnp.float32,
        )
        + jnp.dot(
            spec_imag.reshape(local_rows, group_width),
            chan_sin,
            precision=highest,
            preferred_element_type=jnp.float32,
        )
    ) * norm_scale
    spectrum = mixed_real.astype(jnp.bfloat16)
    returned = lax.all_to_all(
        spectrum.reshape(local_rows, 1, group_width), "row", split_axis=0, concat_axis=1, tiled=True
    )
    returned = returned.reshape(local_rows, group_width)
    output_sum = jnp.dot(
        lax.all_gather(returned, COL, axis=1, tiled=True),
        proj_out,
        preferred_element_type=jnp.float32,
    )
    return output_sum.astype(jnp.bfloat16)


def scaled(value, factor):
    if value is None or abs(factor) < 1e-9:
        return None
    if abs(factor - 1) < 1e-9:
        return value
    if abs(factor + 1) < 1e-9:
        return -value
    return value * np.float32(factor)


def plus(left, right):
    if left is None:
        return right
    return left if right is None else left + right


def minus(left, right):
    if right is None:
        return left
    return -right if left is None else left - right


def complex_scaled(value, angle):
    real, imag = value
    cos, sin = math.cos(angle), math.sin(angle)
    return (
        plus(scaled(real, cos), scaled(imag, sin)),
        minus(scaled(imag, cos), scaled(real, sin)),
    )


def half_transform(values):
    count = len(values)
    half = (count - 1) // 2
    evens = [plus(values[n], values[count - n]) for n in range(1, half + 1)]
    odds = [minus(values[n], values[count - n]) for n in range(1, half + 1)]
    sums = []
    for k in range(count // 2 + 1):
        cos_sum, sin_sum = values[0], None
        if count % 2 == 0:
            cos_sum = plus(cos_sum, scaled(values[count // 2], (-1.0) ** k))
        for n in range(1, half + 1):
            angle = 2 * math.pi * (n * k % count) / count
            cos_sum = plus(cos_sum, scaled(evens[n - 1], math.cos(angle)))
            sin_sum = plus(sin_sum, scaled(odds[n - 1], math.sin(angle)))
        sums.append((cos_sum, sin_sum))
    return sums


def transform(values):
    count = len(values)
    real = half_transform([v[0] for v in values])
    imag = half_transform([v[1] for v in values])
    result = [None] * count
    for k in range(count // 2 + 1):
        (real_cos, real_sin), (imag_cos, imag_sin) = real[k], imag[k]
        result[k] = (plus(real_cos, imag_sin), minus(imag_cos, real_sin))
        if 0 < k < count - k:
            result[count - k] = (minus(real_cos, imag_sin), plus(imag_cos, real_sin))
    return result


def narrow(table):
    return table.astype(jnp.bfloat16)


def split(table):
    high = narrow(table)
    return high, narrow(table - high.astype(np.float64))


def channel_table(width):
    channel = np.arange(width)
    cosines = np.arange(width // 2 + 1)
    sines = np.arange(1, width // 2)
    angle = 2 * math.pi / width
    rows = [
        np.cos(angle * (cosines[:, None] * channel % width)),
        np.sin(angle * (sines[:, None] * channel % width)),
    ]
    return np.concatenate(rows) / math.sqrt(width)


def unpack_table(width):
    table = np.zeros((width, width))
    for k in range(width // 2 + 1):
        table[k, k] = table[k, -k % width] = 1
    for k in range(1, width // 2):
        row = width // 2 + k
        table[row, k], table[row, width - k] = -1, 1
    return table


def project_in(tokens, proj_in):
    rows, width = tokens.shape
    group = proj_in.shape[1]
    high, low = split(channel_table(group))
    tile = next(t for t in (384, 256, 128) if rows % t == 0)

    def body(tokens_ref, proj_ref, high_ref, low_ref, out_ref):
        branch = jnp.dot(
            tokens_ref[...], proj_ref[...], preferred_element_type=jnp.float32
        ).astype(jnp.bfloat16)
        dims = (((1,), (1,)), ((), ()))
        packed = lax.dot_general(
            high_ref[...], branch, dims, preferred_element_type=jnp.float32
        ) + lax.dot_general(low_ref[...], branch, dims, preferred_element_type=jnp.float32)
        out_ref[...] = packed.astype(jnp.bfloat16)

    whole = lambda i: (0, 0)
    return pl.pallas_call(
        body,
        grid=(rows // tile,),
        in_specs=[
            pl.BlockSpec((tile, width), lambda i: (i, 0)),
            pl.BlockSpec((width, group), whole),
            pl.BlockSpec((group, group), whole),
            pl.BlockSpec((group, group), whole),
        ],
        out_specs=pl.BlockSpec((group, tile), lambda i: (0, i)),
        out_shape=jax.ShapeDtypeStruct((group, rows), jnp.bfloat16),
        name="project_in",
    )(tokens, proj_in, jnp.asarray(high), jnp.asarray(low))


def sequence_transform(values, first_packed, group):
    ranks, items, local = values.shape
    tiles = local // LANES
    coarse = ranks * tiles
    length = ranks * local
    blocks = LANES // ranks
    parts = 8
    groups = coarse // parts
    lane = np.arange(LANES)
    twiddle = 2 * math.pi / length * np.arange(coarse)[:, None] * lane
    fine = np.zeros((parts, 2 * LANES, LANES))
    for part in range(parts):
        for rank in range(ranks):
            for block in range(blocks):
                angle = 2 * math.pi / LANES * (lane * (blocks * rank + block) % LANES)
                at = parts * block + (part + rank) % parts
                fine[part, :, at] = np.concatenate([np.cos(angle), np.sin(angle)])
    fine = narrow(fine / math.sqrt(length))

    def body(first_ref, values_ref, cos_ref, sin_ref, fine_ref, out_ref, work_ref):
        packed = first_ref[0] + lax.broadcasted_iota(jnp.int32, (items, LANES), 0)
        turned = packed > group // 2
        outer = []
        for tile in range(tiles):
            at = pl.ds(tile * LANES, LANES)
            outer.append(
                half_transform(
                    [values_ref[rank, :, at].astype(jnp.float32) for rank in range(ranks)]
                )
            )

        def put(c, real, imag):
            cos, sin = cos_ref[c : c + 1, :], sin_ref[c : c + 1, :]
            real, imag = real * cos + imag * sin, imag * cos - real * sin
            real, imag = jnp.where(turned, -imag, real), jnp.where(turned, real, imag)
            part, at = c % parts, pl.ds(c // parts * items, items)
            work_ref[part, at, :LANES] = real.astype(jnp.bfloat16)
            work_ref[part, at, LANES:] = imag.astype(jnp.bfloat16)

        zero = jnp.zeros((items, LANES), jnp.float32)
        for k in range(ranks // 2 + 1):
            column = []
            for tile in range(tiles):
                cos_sum, sin_sum = outer[tile][k]
                column.append(complex_scaled((cos_sum, scaled(sin_sum, -1.0)), 2 * math.pi * k * tile / coarse))
            for m, (real, imag) in enumerate(transform(column)):
                c = k + ranks * m
                mirror = (coarse - c) % coarse
                real = zero if real is None else real
                imag = zero if imag is None else imag
                if mirror % ranks == k and mirror < c:
                    continue
                put(c, real, imag)
                if mirror != c:
                    put(mirror, real, -imag)

        found = [
            jnp.dot(work_ref[part], fine_ref[part], preferred_element_type=jnp.float32)
            for part in range(parts)
        ]
        low_lane = lax.broadcasted_iota(jnp.int32, (groups * items, LANES), 1) % parts
        for rank in range(ranks):
            level = [found[(e - rank) % parts] for e in range(parts)]
            bit = 1
            while len(level) > 1:
                odd = (low_lane & bit) != 0
                level = [jnp.where(odd, b, a) for a, b in zip(level[::2], level[1::2])]
                bit *= 2
            merged = level[0]
            turn = rank % parts
            if turn:
                merged = jnp.where(
                    low_lane < parts - turn,
                    pltpu.roll(merged, LANES - turn, 1),
                    pltpu.roll(merged, parts - turn, 1),
                )
            merged = merged.astype(jnp.bfloat16)
            for tile in range(groups):
                out_ref[rank, :, pl.ds(tile * LANES, LANES)] = merged[tile * items : (tile + 1) * items]

    vmem = pl.BlockSpec(memory_space=pltpu.VMEM)
    return pl.pallas_call(
        body,
        in_specs=[pl.BlockSpec(memory_space=pltpu.SMEM), vmem, vmem, vmem, vmem],
        out_specs=vmem,
        out_shape=jax.ShapeDtypeStruct((ranks, items, local), jnp.bfloat16),
        scratch_shapes=[pltpu.VMEM((parts, groups * items, 2 * LANES), jnp.bfloat16)],
        name="sequence_transform",
    )(
        first_packed,
        values,
        jnp.asarray(np.cos(twiddle), jnp.float32),
        jnp.asarray(np.sin(twiddle), jnp.float32),
        jnp.asarray(fine),
    )


def project_out(pieces, weights, ranks, coarse):
    count = len(pieces)
    group, local = pieces[0].shape
    columns = weights.shape[2]
    blocks = LANES // ranks
    parts = 8
    groups = local // LANES
    step = next(s for s in (3, 2, 1) if groups % s == 0)

    def body(*refs):
        piece_refs, weight_ref, out_ref = refs[:count], refs[count], refs[count + 1]
        total = None
        for at, piece_ref in enumerate(piece_refs):
            part = lax.dot_general(
                piece_ref[...],
                weight_ref[at],
                (((0,), (0,)), ((), ())),
                preferred_element_type=jnp.float32,
            )
            total = part if total is None else total + part
        for at in range(step):
            rows = total[at * LANES : (at + 1) * LANES].astype(jnp.bfloat16)
            out_ref[:, at] = rows.reshape(blocks, parts, columns)

    out = pl.pallas_call(
        body,
        grid=(groups // step,),
        in_specs=[pl.BlockSpec((group, LANES * step), lambda i: (0, i)) for _ in pieces]
        + [pl.BlockSpec(weights.shape, lambda i: (0, 0, 0))],
        out_specs=pl.BlockSpec((blocks, step, parts, columns), lambda i: (0, i, 0, 0)),
        out_shape=jax.ShapeDtypeStruct((blocks, groups, parts, columns), jnp.bfloat16),
        name="project_out",
    )(*pieces, weights)
    return out.reshape(local, columns)


def fast_device(tokens, proj_in, proj_out):
    ranks, far, near = (lax.axis_size(a) for a in (ROW, *COL))
    local = tokens.shape[0]
    group = proj_in.shape[1]
    items = group // ranks
    columns = proj_out.shape[1]
    rank, own = lax.axis_index(ROW), lax.axis_index(COL)
    packed = project_in(tokens, proj_in).reshape(ranks, items, local)
    values = lax.all_to_all(packed, ROW, split_axis=0, concat_axis=0, tiled=True)
    first = (rank * items).astype(jnp.int32).reshape(1)
    found = sequence_transform(values, first, group)
    back = lax.all_to_all(found, ROW, split_axis=0, concat_axis=0, tiled=True)
    pieces = [back.reshape(group, local)]
    order = [own]
    for axis, size, stride in ((COL[0], far, near), (COL[1], near, 1)):
        for piece in list(pieces):
            pieces.append(lax.ppermute(piece, axis, [(i, i ^ 1) for i in range(size)]))
        order += [o ^ stride for o in order]
    groups = jnp.dot(
        jnp.asarray(narrow(unpack_table(group))),
        jnp.concatenate([lax.dynamic_slice_in_dim(proj_out, o * group, group, 0) for o in order], 1),
        preferred_element_type=jnp.float32,
    ).astype(jnp.bfloat16)
    weights = groups.reshape(group, len(order), columns).transpose(1, 0, 2)
    return project_out(pieces, weights, ranks, ranks * (local // LANES))


def solution(mesh):
    ranks, cols = mesh.devices.shape
    near = 2 if cols % 2 == 0 else 1
    inner = Mesh(mesh.devices.reshape(ranks, cols // near, near), (ROW, *COL))

    def program(tokens, proj_in, proj_out):
        local, group = tokens.shape[0] // ranks, proj_in.shape[1] // cols
        fits = (
            group == LANES
            and LANES % ranks == 0
            and ranks % 8 == 0
            and local % LANES == 0
            and near == 2
            and cols == 4
        )
        return jax.shard_map(
            fast_device if fits else general_device,
            mesh=inner,
            in_specs=(P(ROW, None), P(None, COL), P(None, COL)),
            out_specs=P(ROW, COL),
            check_vma=False,
        )(tokens, proj_in, proj_out)

    return program
```

```python
import math

import jax
import jax.numpy as jnp
import numpy as np
from jax import lax
from jax.experimental import pallas as pl
from jax.experimental.pallas import tpu as pltpu
from jax.sharding import Mesh, PartitionSpec as P

LANES = 128
ROW = "row"
COL = ("far", "near")
CHUNKS = 1


def cos_sin(row_ids, col_ids, period):
    phase_idx = row_ids * col_ids % period
    angles = phase_idx.astype(jnp.float32) * (2.0 * math.pi / period)
    return (jnp.cos(angles), jnp.sin(angles))


def apply_table(form, table_cos, table_sin, real_part, imag_part):
    highest = lax.Precision.HIGHEST
    out_real = jnp.einsum(form, table_cos, real_part, precision=highest) + jnp.einsum(
        form, table_sin, imag_part, precision=highest
    )
    out_imag = jnp.einsum(form, table_cos, imag_part, precision=highest) - jnp.einsum(
        form, table_sin, real_part, precision=highest
    )
    return (out_real, out_imag)


def general_device(tokens, proj_in, proj_out):
    row_count = lax.axis_size(ROW)
    local_rows = tokens.shape[0]
    group_width = proj_in.shape[1]
    seq_length = local_rows * row_count
    row_rank = lax.axis_index(ROW)
    highest = lax.Precision.HIGHEST
    first_len = 16
    second_len = local_rows // first_len
    branch_in = jnp.dot(tokens, proj_in, preferred_element_type=jnp.float32).astype(jnp.bfloat16)
    outer_idx = jnp.arange(row_count, dtype=jnp.int32)
    outer_cos, outer_sin = cos_sin(outer_idx[:, None], outer_idx[None, :], row_count)
    values = lax.all_to_all(
        branch_in.reshape(1, local_rows, group_width),
        "row",
        split_axis=1,
        concat_axis=0,
        tiled=True,
    ).astype(jnp.float32)
    real_part = jnp.einsum("kn,nmg->kmg", outer_cos, values, precision=highest)
    imag_part = -jnp.einsum("kn,nmg->kmg", outer_sin, values, precision=highest)
    real_parts = real_part
    imag_parts = imag_part
    inner_idx = jnp.arange(local_rows, dtype=jnp.int32)
    first_idx = jnp.arange(first_len, dtype=jnp.int32)
    second_idx = jnp.arange(second_len, dtype=jnp.int32)
    first_cos, first_sin = cos_sin(first_idx[:, None], first_idx[None, :], first_len)
    second_cos, second_sin = cos_sin(second_idx[:, None], second_idx[None, :], second_len)
    mid_cos, mid_sin = cos_sin(first_idx[:, None], second_idx[None, :], local_rows)
    mid_cos = mid_cos[None, :, :, None]
    mid_sin = mid_sin[None, :, :, None]
    twid_cos, twid_sin = cos_sin(row_rank, inner_idx, seq_length)
    twid_cos = twid_cos[None, :, None]
    twid_sin = twid_sin[None, :, None]
    real_part = lax.all_to_all(real_parts, "row", split_axis=0, concat_axis=1, tiled=True)
    imag_part = lax.all_to_all(imag_parts, "row", split_axis=0, concat_axis=1, tiled=True)
    real_part, imag_part = (
        real_part * twid_cos + imag_part * twid_sin,
        imag_part * twid_cos - real_part * twid_sin,
    )
    leading = real_part.shape[0]
    items = real_part.shape[2]
    real_part = real_part.reshape(leading, first_len, second_len, items)
    imag_part = imag_part.reshape(leading, first_len, second_len, items)
    real_part, imag_part = apply_table("kn,anqg->akqg", first_cos, first_sin, real_part, imag_part)
    real_part, imag_part = (
        real_part * mid_cos + imag_part * mid_sin,
        imag_part * mid_cos - real_part * mid_sin,
    )
    real_part, imag_part = apply_table(
        "kq,apqg->akpg", second_cos, second_sin, real_part, imag_part
    )
    spec_real = real_part.reshape(leading, local_rows, items)
    spec_imag = imag_part.reshape(leading, local_rows, items)
    channel = jnp.arange(group_width, dtype=jnp.int32)
    chan_cos, chan_sin = cos_sin(channel[:, None], channel[None, :], group_width)
    norm_scale = 1.0 / math.sqrt(seq_length * group_width)
    mixed_real = (
        jnp.dot(
            spec_real.reshape(local_rows, group_width),
            chan_cos,
            precision=highest,
            preferred_element_type=jnp.float32,
        )
        + jnp.dot(
            spec_imag.reshape(local_rows, group_width),
            chan_sin,
            precision=highest,
            preferred_element_type=jnp.float32,
        )
    ) * norm_scale
    spectrum = mixed_real.astype(jnp.bfloat16)
    returned = lax.all_to_all(
        spectrum.reshape(local_rows, 1, group_width), "row", split_axis=0, concat_axis=1, tiled=True
    )
    returned = returned.reshape(local_rows, group_width)
    output_sum = jnp.dot(
        lax.all_gather(returned, COL, axis=1, tiled=True),
        proj_out,
        preferred_element_type=jnp.float32,
    )
    return output_sum.astype(jnp.bfloat16)


def scaled(value, factor):
    if value is None or abs(factor) < 1e-9:
        return None
    if abs(factor - 1) < 1e-9:
        return value
    if abs(factor + 1) < 1e-9:
        return -value
    return value * np.float32(factor)


def plus(left, right):
    if left is None:
        return right
    return left if right is None else left + right


def minus(left, right):
    if right is None:
        return left
    return -right if left is None else left - right


def complex_scaled(value, angle):
    real, imag = value
    cos, sin = math.cos(angle), math.sin(angle)
    return (
        plus(scaled(real, cos), scaled(imag, sin)),
        minus(scaled(imag, cos), scaled(real, sin)),
    )


def half_transform(values):
    count = len(values)
    half = (count - 1) // 2
    evens = [plus(values[n], values[count - n]) for n in range(1, half + 1)]
    odds = [minus(values[n], values[count - n]) for n in range(1, half + 1)]
    sums = []
    for k in range(count // 2 + 1):
        cos_sum, sin_sum = values[0], None
        if count % 2 == 0:
            cos_sum = plus(cos_sum, scaled(values[count // 2], (-1.0) ** k))
        for n in range(1, half + 1):
            angle = 2 * math.pi * (n * k % count) / count
            cos_sum = plus(cos_sum, scaled(evens[n - 1], math.cos(angle)))
            sin_sum = plus(sin_sum, scaled(odds[n - 1], math.sin(angle)))
        sums.append((cos_sum, sin_sum))
    return sums


def transform(values):
    count = len(values)
    real = half_transform([v[0] for v in values])
    imag = half_transform([v[1] for v in values])
    result = [None] * count
    for k in range(count // 2 + 1):
        (real_cos, real_sin), (imag_cos, imag_sin) = real[k], imag[k]
        result[k] = (plus(real_cos, imag_sin), minus(imag_cos, real_sin))
        if 0 < k < count - k:
            result[count - k] = (minus(real_cos, imag_sin), plus(imag_cos, real_sin))
    return result


def narrow(table):
    return table.astype(jnp.bfloat16)


def split(table):
    high = narrow(table)
    return high, narrow(table - high.astype(np.float64))


def channel_table(width):
    channel = np.arange(width)
    cosines = np.arange(width // 2 + 1)
    sines = np.arange(1, width // 2)
    angle = 2 * math.pi / width
    rows = [
        np.cos(angle * (cosines[:, None] * channel % width)),
        np.sin(angle * (sines[:, None] * channel % width)),
    ]
    return np.concatenate(rows) / math.sqrt(width)


def unpack_table(width, ranks, chunks):
    table = np.zeros((width, width))
    for k in range(width // 2 + 1):
        table[k, k] = table[k, -k % width] = 1
    for k in range(1, width // 2):
        row = width // 2 + k
        table[row, k], table[row, width - k] = -1, 1
    table = table.reshape(ranks, chunks, -1, width).transpose(1, 0, 2, 3)
    return table.reshape(width, width)


def in_vmem(array):
    return pltpu.with_memory_space_constraint(array, pltpu.VMEM)


def in_hbm(array):
    return pltpu.with_memory_space_constraint(array, pltpu.HBM)


VMEM_SPEC = pl.BlockSpec(memory_space=pltpu.VMEM)
SMEM_SPEC = pl.BlockSpec(memory_space=pltpu.SMEM)
PARAMS = pltpu.CompilerParams(vmem_limit_bytes=32 * 2**20)


def project_in(tokens, proj_in):
    rows, width = tokens.shape
    group = proj_in.shape[1]
    high, low = split(channel_table(group))
    steps = 2 if width % 256 == 0 else 1
    depth = width // steps

    def body(tokens_ref, proj_ref, high_ref, low_ref, out_ref, sum_ref):
        step = pl.program_id(0)
        part = jnp.dot(
            tokens_ref[...], proj_ref[...], preferred_element_type=jnp.float32
        )

        @pl.when(step == 0)
        def _():
            sum_ref[...] = part

        @pl.when(step > 0)
        def _():
            sum_ref[...] += part

        @pl.when(step == steps - 1)
        def _():
            branch = sum_ref[...].astype(jnp.bfloat16)
            dims = (((1,), (1,)), ((), ()))
            packed = lax.dot_general(
                high_ref[...], branch, dims, preferred_element_type=jnp.float32
            ) + lax.dot_general(low_ref[...], branch, dims, preferred_element_type=jnp.float32)
            out_ref[...] = packed.astype(jnp.bfloat16)

    whole = lambda i: (0, 0)
    return pl.pallas_call(
        body,
        grid=(steps,),
        in_specs=[
            pl.BlockSpec((rows, depth), lambda i: (0, i)),
            pl.BlockSpec((depth, group), lambda i: (i, 0)),
            pl.BlockSpec((group, group), whole),
            pl.BlockSpec((group, group), whole),
        ],
        out_specs=pl.BlockSpec((group, rows), whole),
        out_shape=jax.ShapeDtypeStruct((group, rows), jnp.bfloat16),
        scratch_shapes=[pltpu.VMEM((rows, group), jnp.float32)],
        compiler_params=PARAMS,
        name="project_in",
    )(*map(in_hbm, (tokens, proj_in, jnp.asarray(high), jnp.asarray(low))))


def sequence_transform(values, first_packed, group, chunk, chunks):
    ranks, items, local = values.shape
    items //= chunks
    offset = chunk * items
    tiles = local // LANES
    coarse = ranks * tiles
    length = ranks * local
    blocks = LANES // ranks
    parts = 8
    groups = coarse // parts
    lane = np.arange(LANES)
    twiddle = 2 * math.pi / length * np.arange(coarse)[:, None] * lane
    fine = np.zeros((parts, 2 * LANES, LANES))
    for part in range(parts):
        for rank in range(ranks):
            for block in range(blocks):
                angle = 2 * math.pi / LANES * (lane * (blocks * rank + block) % LANES)
                at = parts * block + (part + rank) % parts
                fine[part, :, at] = np.concatenate([np.cos(angle), np.sin(angle)])
    fine = narrow(fine / math.sqrt(length))

    def body(first_ref, values_ref, cos_ref, sin_ref, fine_ref, out_ref, work_ref):
        packed = first_ref[0] + offset + lax.broadcasted_iota(jnp.int32, (items, LANES), 0)
        turned = packed > group // 2
        outer = []
        for tile in range(tiles):
            at = pl.ds(tile * LANES, LANES)
            outer.append(
                half_transform(
                    [values_ref[rank, offset : offset + items, at].astype(jnp.float32) for rank in range(ranks)]
                )
            )

        def put(c, real, imag):
            cos, sin = cos_ref[c : c + 1, :], sin_ref[c : c + 1, :]
            real, imag = real * cos + imag * sin, imag * cos - real * sin
            real, imag = jnp.where(turned, -imag, real), jnp.where(turned, real, imag)
            part, at = c % parts, pl.ds(c // parts * items, items)
            work_ref[part, at, :LANES] = real.astype(jnp.bfloat16)
            work_ref[part, at, LANES:] = imag.astype(jnp.bfloat16)

        zero = jnp.zeros((items, LANES), jnp.float32)
        for k in range(ranks // 2 + 1):
            column = []
            for tile in range(tiles):
                cos_sum, sin_sum = outer[tile][k]
                column.append(complex_scaled((cos_sum, scaled(sin_sum, -1.0)), 2 * math.pi * k * tile / coarse))
            for m, (real, imag) in enumerate(transform(column)):
                c = k + ranks * m
                mirror = (coarse - c) % coarse
                real = zero if real is None else real
                imag = zero if imag is None else imag
                if mirror % ranks == k and mirror < c:
                    continue
                put(c, real, imag)
                if mirror != c:
                    put(mirror, real, -imag)

        found = [
            jnp.dot(work_ref[part], fine_ref[part], preferred_element_type=jnp.float32)
            for part in range(parts)
        ]
        low_lane = lax.broadcasted_iota(jnp.int32, (groups * items, LANES), 1) % parts
        for rank in range(ranks):
            level = [found[(e - rank) % parts] for e in range(parts)]
            bit = 1
            while len(level) > 1:
                odd = (low_lane & bit) != 0
                level = [jnp.where(odd, b, a) for a, b in zip(level[::2], level[1::2])]
                bit *= 2
            merged = level[0]
            turn = rank % parts
            if turn:
                merged = jnp.where(
                    low_lane < parts - turn,
                    pltpu.roll(merged, LANES - turn, 1),
                    pltpu.roll(merged, parts - turn, 1),
                )
            merged = merged.astype(jnp.bfloat16)
            for tile in range(groups):
                out_ref[rank, :, pl.ds(tile * LANES, LANES)] = merged[tile * items : (tile + 1) * items]

    return pl.pallas_call(
        body,
        in_specs=[SMEM_SPEC] + [VMEM_SPEC] * 4,
        out_specs=VMEM_SPEC,
        out_shape=pltpu.VMEM((ranks, items, local), jnp.bfloat16),
        scratch_shapes=[pltpu.VMEM((parts, groups * items, 2 * LANES), jnp.bfloat16)],
        compiler_params=PARAMS,
        name="sequence_transform",
    )(
        first_packed,
        in_vmem(values),
        in_vmem(jnp.asarray(np.cos(twiddle), jnp.float32)),
        in_vmem(jnp.asarray(np.sin(twiddle), jnp.float32)),
        in_vmem(jnp.asarray(fine)),
    )


def fold_weights(proj_out, order, group, ranks, chunks):
    count, columns = len(order), proj_out.shape[1]
    table = narrow(unpack_table(group, ranks, chunks))

    def body(order_ref, proj_ref, table_ref, out_ref):
        for at in range(count):
            rows = proj_ref[pl.ds(pl.multiple_of(order_ref[at] * group, group), group), :]
            folded = jnp.dot(table_ref[...], rows, preferred_element_type=jnp.float32)
            out_ref[at * group : (at + 1) * group, :] = folded.astype(jnp.bfloat16)

    return pl.pallas_call(
        body,
        in_specs=[SMEM_SPEC, VMEM_SPEC, VMEM_SPEC],
        out_specs=VMEM_SPEC,
        out_shape=pltpu.VMEM((count * group, columns), jnp.bfloat16),
        compiler_params=PARAMS,
        name="fold_weights",
    )(jnp.stack(order).astype(jnp.int32), in_vmem(proj_out), jnp.asarray(table))


def add_pieces(pieces, weights, first, total, blocks, last):
    count = len(pieces)
    depth = sum(piece.shape[0] for piece in pieces)
    local = pieces[0].shape[1]
    columns = weights.shape[1]
    parts = 8
    groups = local // LANES
    step = next(s for s in (3, 2, 1) if groups % s == 0)
    width = LANES * step

    def body(*refs):
        piece_refs, weight_ref = refs[:count], refs[count]
        out_ref = refs[-1]
        at = pl.ds(pl.multiple_of(pl.program_id(0) * width, width), width)
        lhs = jnp.concatenate([r[:, at] for r in piece_refs], 0)
        rhs = weight_ref[first : first + depth]
        part = lax.dot_general(
            lhs, rhs, (((0,), (0,)), ((), ())), preferred_element_type=jnp.float32
        )
        if total is not None:
            part = part + refs[count + 1][at, :]
        if last:
            for tile in range(step):
                rows = part[tile * LANES : (tile + 1) * LANES].astype(jnp.bfloat16)
                out_ref[:, tile] = rows.reshape(blocks, parts, columns)
        else:
            out_ref[at, :] = part

    if last:
        out_spec = pl.BlockSpec((blocks, step, parts, columns), lambda i: (0, i, 0, 0))
        out_shape = jax.ShapeDtypeStruct((blocks, groups, parts, columns), jnp.bfloat16)
    else:
        out_spec, out_shape = VMEM_SPEC, pltpu.VMEM((local, columns), jnp.float32)
    inputs = [*pieces, weights] + ([] if total is None else [total])
    return pl.pallas_call(
        body,
        grid=(groups // step,),
        in_specs=[VMEM_SPEC] * len(inputs),
        out_specs=out_spec,
        out_shape=out_shape,
        compiler_params=PARAMS,
        name="finish_pieces" if last else "add_pieces",
    )(*map(in_vmem, inputs))


def fast_device(tokens, proj_in, proj_out):
    ranks, _, near = (lax.axis_size(a) for a in (ROW, *COL))
    local = tokens.shape[0]
    group = proj_in.shape[1]
    items = group // ranks
    columns = proj_out.shape[1]
    rank, own = lax.axis_index(ROW), lax.axis_index(COL)
    order = [own, own ^ 1, own ^ near, own ^ near ^ 1]
    blocks = LANES // ranks
    swap = [(i, i ^ 1) for i in range(2)]
    packed = project_in(tokens, proj_in).reshape(ranks, items, local)
    values = lax.all_to_all(packed, ROW, split_axis=0, concat_axis=0, tiled=True)
    first = (rank * items).astype(jnp.int32).reshape(1)
    weights = fold_weights(proj_out, order, group, ranks, CHUNKS)
    found = []
    for c in range(CHUNKS):
        found.append(sequence_transform(values, first, group, c, CHUNKS))
    here, there, here_too, there_too = [], [], [], []
    for c in range(CHUNKS):
        back = lax.all_to_all(found[c], ROW, split_axis=0, concat_axis=0, tiled=True)
        here.append(back.reshape(-1, local))
        there.append(lax.ppermute(here[c], COL[0], swap))
        here_too.append(lax.ppermute(here[c], COL[1], swap))
    total = add_pieces([*here, *here_too], weights, 0, None, blocks, False)
    for c in range(CHUNKS):
        there_too.append(lax.ppermute(there[c], COL[1], swap))
    out = add_pieces([*there, *there_too], weights, 2 * group, total, blocks, True)
    return out.reshape(local, columns)


def solution(mesh):
    ranks, cols = mesh.devices.shape
    near = 2 if cols % 2 == 0 else 1
    inner = Mesh(mesh.devices.reshape(ranks, cols // near, near), (ROW, *COL))

    def program(tokens, proj_in, proj_out):
        local, group = tokens.shape[0] // ranks, proj_in.shape[1] // cols
        fits = (
            group == LANES
            and LANES % ranks == 0
            and ranks % 8 == 0
            and local % LANES == 0
            and near == 2
            and cols == 4
        )
        step = jax.shard_map(
            fast_device if fits else general_device,
            mesh=inner,
            in_specs=(P(ROW, None), P(None, COL), P(None, COL)),
            out_specs=P(ROW, COL),
            check_vma=False,
        )
        return step(tokens, proj_in, proj_out)

    return program
```

```python
import math

import jax
import jax.numpy as jnp
import numpy as np
from jax import lax
from jax.experimental import pallas as pl
from jax.experimental.pallas import tpu as pltpu
from jax.sharding import Mesh, PartitionSpec as P

LANES = 128
ROW = "row"
COL = ("far", "near")
CHUNKS = 1


def cos_sin(row_ids, col_ids, period):
    phase_idx = row_ids * col_ids % period
    angles = phase_idx.astype(jnp.float32) * (2.0 * math.pi / period)
    return (jnp.cos(angles), jnp.sin(angles))


def apply_table(form, table_cos, table_sin, real_part, imag_part):
    highest = lax.Precision.HIGHEST
    out_real = jnp.einsum(form, table_cos, real_part, precision=highest) + jnp.einsum(
        form, table_sin, imag_part, precision=highest
    )
    out_imag = jnp.einsum(form, table_cos, imag_part, precision=highest) - jnp.einsum(
        form, table_sin, real_part, precision=highest
    )
    return (out_real, out_imag)


def general_device(tokens, proj_in, proj_out):
    row_count = lax.axis_size(ROW)
    local_rows = tokens.shape[0]
    group_width = proj_in.shape[1]
    seq_length = local_rows * row_count
    row_rank = lax.axis_index(ROW)
    highest = lax.Precision.HIGHEST
    first_len = 16
    second_len = local_rows // first_len
    branch_in = jnp.dot(tokens, proj_in, preferred_element_type=jnp.float32).astype(jnp.bfloat16)
    outer_idx = jnp.arange(row_count, dtype=jnp.int32)
    outer_cos, outer_sin = cos_sin(outer_idx[:, None], outer_idx[None, :], row_count)
    values = lax.all_to_all(
        branch_in.reshape(1, local_rows, group_width),
        "row",
        split_axis=1,
        concat_axis=0,
        tiled=True,
    ).astype(jnp.float32)
    real_part = jnp.einsum("kn,nmg->kmg", outer_cos, values, precision=highest)
    imag_part = -jnp.einsum("kn,nmg->kmg", outer_sin, values, precision=highest)
    real_parts = real_part
    imag_parts = imag_part
    inner_idx = jnp.arange(local_rows, dtype=jnp.int32)
    first_idx = jnp.arange(first_len, dtype=jnp.int32)
    second_idx = jnp.arange(second_len, dtype=jnp.int32)
    first_cos, first_sin = cos_sin(first_idx[:, None], first_idx[None, :], first_len)
    second_cos, second_sin = cos_sin(second_idx[:, None], second_idx[None, :], second_len)
    mid_cos, mid_sin = cos_sin(first_idx[:, None], second_idx[None, :], local_rows)
    mid_cos = mid_cos[None, :, :, None]
    mid_sin = mid_sin[None, :, :, None]
    twid_cos, twid_sin = cos_sin(row_rank, inner_idx, seq_length)
    twid_cos = twid_cos[None, :, None]
    twid_sin = twid_sin[None, :, None]
    real_part = lax.all_to_all(real_parts, "row", split_axis=0, concat_axis=1, tiled=True)
    imag_part = lax.all_to_all(imag_parts, "row", split_axis=0, concat_axis=1, tiled=True)
    real_part, imag_part = (
        real_part * twid_cos + imag_part * twid_sin,
        imag_part * twid_cos - real_part * twid_sin,
    )
    leading = real_part.shape[0]
    items = real_part.shape[2]
    real_part = real_part.reshape(leading, first_len, second_len, items)
    imag_part = imag_part.reshape(leading, first_len, second_len, items)
    real_part, imag_part = apply_table("kn,anqg->akqg", first_cos, first_sin, real_part, imag_part)
    real_part, imag_part = (
        real_part * mid_cos + imag_part * mid_sin,
        imag_part * mid_cos - real_part * mid_sin,
    )
    real_part, imag_part = apply_table(
        "kq,apqg->akpg", second_cos, second_sin, real_part, imag_part
    )
    spec_real = real_part.reshape(leading, local_rows, items)
    spec_imag = imag_part.reshape(leading, local_rows, items)
    channel = jnp.arange(group_width, dtype=jnp.int32)
    chan_cos, chan_sin = cos_sin(channel[:, None], channel[None, :], group_width)
    norm_scale = 1.0 / math.sqrt(seq_length * group_width)
    mixed_real = (
        jnp.dot(
            spec_real.reshape(local_rows, group_width),
            chan_cos,
            precision=highest,
            preferred_element_type=jnp.float32,
        )
        + jnp.dot(
            spec_imag.reshape(local_rows, group_width),
            chan_sin,
            precision=highest,
            preferred_element_type=jnp.float32,
        )
    ) * norm_scale
    spectrum = mixed_real.astype(jnp.bfloat16)
    returned = lax.all_to_all(
        spectrum.reshape(local_rows, 1, group_width), "row", split_axis=0, concat_axis=1, tiled=True
    )
    returned = returned.reshape(local_rows, group_width)
    output_sum = jnp.dot(
        lax.all_gather(returned, COL, axis=1, tiled=True),
        proj_out,
        preferred_element_type=jnp.float32,
    )
    return output_sum.astype(jnp.bfloat16)


def scaled(value, factor):
    if value is None or abs(factor) < 1e-9:
        return None
    if abs(factor - 1) < 1e-9:
        return value
    if abs(factor + 1) < 1e-9:
        return -value
    return value * np.float32(factor)


def plus(left, right):
    if left is None:
        return right
    return left if right is None else left + right


def minus(left, right):
    if right is None:
        return left
    return -right if left is None else left - right


def complex_scaled(value, angle):
    real, imag = value
    cos, sin = math.cos(angle), math.sin(angle)
    return (
        plus(scaled(real, cos), scaled(imag, sin)),
        minus(scaled(imag, cos), scaled(real, sin)),
    )


def half_transform(values):
    count = len(values)
    half = (count - 1) // 2
    evens = [plus(values[n], values[count - n]) for n in range(1, half + 1)]
    odds = [minus(values[n], values[count - n]) for n in range(1, half + 1)]
    sums = []
    for k in range(count // 2 + 1):
        cos_sum, sin_sum = values[0], None
        if count % 2 == 0:
            cos_sum = plus(cos_sum, scaled(values[count // 2], (-1.0) ** k))
        for n in range(1, half + 1):
            angle = 2 * math.pi * (n * k % count) / count
            cos_sum = plus(cos_sum, scaled(evens[n - 1], math.cos(angle)))
            sin_sum = plus(sin_sum, scaled(odds[n - 1], math.sin(angle)))
        sums.append((cos_sum, sin_sum))
    return sums


def transform(values):
    count = len(values)
    real = half_transform([v[0] for v in values])
    imag = half_transform([v[1] for v in values])
    result = [None] * count
    for k in range(count // 2 + 1):
        (real_cos, real_sin), (imag_cos, imag_sin) = real[k], imag[k]
        result[k] = (plus(real_cos, imag_sin), minus(imag_cos, real_sin))
        if 0 < k < count - k:
            result[count - k] = (minus(real_cos, imag_sin), plus(imag_cos, real_sin))
    return result


def narrow(table):
    return table.astype(jnp.bfloat16)


def split(table):
    high = narrow(table)
    return high, narrow(table - high.astype(np.float64))


def channel_table(width):
    channel = np.arange(width)
    cosines = np.arange(width // 2 + 1)
    sines = np.arange(1, width // 2)
    angle = 2 * math.pi / width
    rows = [
        np.cos(angle * (cosines[:, None] * channel % width)),
        np.sin(angle * (sines[:, None] * channel % width)),
    ]
    return np.concatenate(rows) / math.sqrt(width)


def unpack_table(width, ranks, chunks):
    table = np.zeros((width, width))
    for k in range(width // 2 + 1):
        table[k, k] = table[k, -k % width] = 1
    for k in range(1, width // 2):
        row = width // 2 + k
        table[row, k], table[row, width - k] = -1, 1
    table = table.reshape(ranks, chunks, -1, width).transpose(1, 0, 2, 3)
    return table.reshape(width, width)


def in_vmem(array):
    return pltpu.with_memory_space_constraint(array, pltpu.VMEM)


def in_hbm(array):
    return pltpu.with_memory_space_constraint(array, pltpu.HBM)


VMEM_SPEC = pl.BlockSpec(memory_space=pltpu.VMEM)
SMEM_SPEC = pl.BlockSpec(memory_space=pltpu.SMEM)
PARAMS = pltpu.CompilerParams(vmem_limit_bytes=32 * 2**20)


def project_in(tokens, proj_in):
    rows, width = tokens.shape
    group = proj_in.shape[1]
    high, low = split(channel_table(group))
    steps = 2 if width % 256 == 0 else 1
    depth = width // steps

    def body(tokens_ref, proj_ref, high_ref, low_ref, out_ref, sum_ref):
        step = pl.program_id(0)
        part = jnp.dot(
            tokens_ref[...], proj_ref[...], preferred_element_type=jnp.float32
        )

        @pl.when(step == 0)
        def _():
            sum_ref[...] = part

        @pl.when(step > 0)
        def _():
            sum_ref[...] += part

        @pl.when(step == steps - 1)
        def _():
            branch = sum_ref[...].astype(jnp.bfloat16)
            dims = (((1,), (1,)), ((), ()))
            packed = lax.dot_general(
                high_ref[...], branch, dims, preferred_element_type=jnp.float32
            ) + lax.dot_general(low_ref[...], branch, dims, preferred_element_type=jnp.float32)
            out_ref[...] = packed.astype(jnp.bfloat16)

    whole = lambda i: (0, 0)
    return pl.pallas_call(
        body,
        grid=(steps,),
        in_specs=[
            pl.BlockSpec((rows, depth), lambda i: (0, i)),
            pl.BlockSpec((depth, group), lambda i: (i, 0)),
            pl.BlockSpec((group, group), whole),
            pl.BlockSpec((group, group), whole),
        ],
        out_specs=VMEM_SPEC,
        out_shape=pltpu.VMEM((group, rows), jnp.bfloat16),
        scratch_shapes=[pltpu.VMEM((rows, group), jnp.float32)],
        compiler_params=PARAMS,
        name="project_in",
    )(*map(in_hbm, (tokens, proj_in, jnp.asarray(high), jnp.asarray(low))))


def sequence_transform(values, first_packed, group, chunk, chunks):
    ranks, items, local = values.shape
    items //= chunks
    offset = chunk * items
    tiles = local // LANES
    coarse = ranks * tiles
    length = ranks * local
    blocks = LANES // ranks
    parts = 8
    groups = coarse // parts
    lane = np.arange(LANES)
    twiddle = 2 * math.pi / length * np.arange(coarse)[:, None] * lane
    fine = np.zeros((parts, 2 * LANES, LANES))
    for part in range(parts):
        for rank in range(ranks):
            for block in range(blocks):
                angle = 2 * math.pi / LANES * (lane * (blocks * rank + block) % LANES)
                at = parts * block + (part + rank) % parts
                fine[part, :, at] = np.concatenate([np.cos(angle), np.sin(angle)])
    fine = narrow(fine / math.sqrt(length))

    def body(first_ref, values_ref, cos_ref, sin_ref, fine_ref, out_ref, work_ref):
        packed = first_ref[0] + offset + lax.broadcasted_iota(jnp.int32, (items, LANES), 0)
        turned = packed > group // 2
        outer = []
        for tile in range(tiles):
            at = pl.ds(tile * LANES, LANES)
            outer.append(
                half_transform(
                    [values_ref[rank, offset : offset + items, at].astype(jnp.float32) for rank in range(ranks)]
                )
            )

        def put(c, real, imag):
            cos, sin = cos_ref[c : c + 1, :], sin_ref[c : c + 1, :]
            real, imag = real * cos + imag * sin, imag * cos - real * sin
            real, imag = jnp.where(turned, -imag, real), jnp.where(turned, real, imag)
            part, at = c % parts, pl.ds(c // parts * items, items)
            work_ref[part, at, :LANES] = real.astype(jnp.bfloat16)
            work_ref[part, at, LANES:] = imag.astype(jnp.bfloat16)

        zero = jnp.zeros((items, LANES), jnp.float32)
        for k in range(ranks // 2 + 1):
            column = []
            for tile in range(tiles):
                cos_sum, sin_sum = outer[tile][k]
                column.append(complex_scaled((cos_sum, scaled(sin_sum, -1.0)), 2 * math.pi * k * tile / coarse))
            for m, (real, imag) in enumerate(transform(column)):
                c = k + ranks * m
                mirror = (coarse - c) % coarse
                real = zero if real is None else real
                imag = zero if imag is None else imag
                if mirror % ranks == k and mirror < c:
                    continue
                put(c, real, imag)
                if mirror != c:
                    put(mirror, real, -imag)

        found = [
            jnp.dot(work_ref[part], fine_ref[part], preferred_element_type=jnp.float32)
            for part in range(parts)
        ]
        low_lane = lax.broadcasted_iota(jnp.int32, (groups * items, LANES), 1) % parts
        for rank in range(ranks):
            level = [found[(e - rank) % parts] for e in range(parts)]
            bit = 1
            while len(level) > 1:
                odd = (low_lane & bit) != 0
                level = [jnp.where(odd, b, a) for a, b in zip(level[::2], level[1::2])]
                bit *= 2
            merged = level[0]
            turn = rank % parts
            if turn:
                merged = jnp.where(
                    low_lane < parts - turn,
                    pltpu.roll(merged, LANES - turn, 1),
                    pltpu.roll(merged, parts - turn, 1),
                )
            merged = merged.astype(jnp.bfloat16)
            for tile in range(groups):
                out_ref[rank, :, pl.ds(tile * LANES, LANES)] = merged[tile * items : (tile + 1) * items]

    return pl.pallas_call(
        body,
        in_specs=[SMEM_SPEC] + [VMEM_SPEC] * 4,
        out_specs=VMEM_SPEC,
        out_shape=pltpu.VMEM((ranks, items, local), jnp.bfloat16),
        scratch_shapes=[pltpu.VMEM((parts, groups * items, 2 * LANES), jnp.bfloat16)],
        compiler_params=PARAMS,
        name="sequence_transform",
    )(
        first_packed,
        in_vmem(values),
        in_vmem(jnp.asarray(np.cos(twiddle), jnp.float32)),
        in_vmem(jnp.asarray(np.sin(twiddle), jnp.float32)),
        in_vmem(jnp.asarray(fine)),
    )


def fold_weights(proj_out, order, group, ranks, chunks):
    count, columns = len(order), proj_out.shape[1]
    table = narrow(unpack_table(group, ranks, chunks))

    def body(order_ref, proj_ref, table_ref, out_ref):
        for at in range(count):
            rows = proj_ref[pl.ds(pl.multiple_of(order_ref[at] * group, group), group), :]
            folded = jnp.dot(table_ref[...], rows, preferred_element_type=jnp.float32)
            out_ref[at * group : (at + 1) * group, :] = folded.astype(jnp.bfloat16)

    return pl.pallas_call(
        body,
        in_specs=[SMEM_SPEC, VMEM_SPEC, VMEM_SPEC],
        out_specs=VMEM_SPEC,
        out_shape=pltpu.VMEM((count * group, columns), jnp.bfloat16),
        compiler_params=PARAMS,
        name="fold_weights",
    )(jnp.stack(order).astype(jnp.int32), in_vmem(proj_out), jnp.asarray(table))


def add_pieces(pieces, weights, first, total, blocks, last):
    count = len(pieces)
    depth = sum(piece.shape[0] for piece in pieces)
    local = pieces[0].shape[1]
    columns = weights.shape[1]
    parts = 8
    groups = local // LANES

    def product(refs, at):
        lhs = jnp.concatenate([r[:, at] for r in refs[:count]], 0)
        rhs = refs[count][first : first + depth]
        return lax.dot_general(
            lhs, rhs, (((0,), (0,)), ((), ())), preferred_element_type=jnp.float32
        )

    def start(*refs):
        for tile in range(groups):
            at = pl.ds(tile * LANES, LANES)
            refs[-1][at, :] = product(refs, at)

    def finish(*refs):
        total_ref, out_ref, rows_ref, sem_ref = refs[-4:]
        copies = []
        for tile in range(groups):
            at = pl.ds(tile * LANES, LANES)
            rows = (product(refs, at) + total_ref[at, :]).astype(jnp.bfloat16)
            rows_ref[tile] = rows.reshape(blocks, parts, columns)
            copies.append(
                pltpu.make_async_copy(rows_ref.at[tile], out_ref.at[:, tile], sem_ref.at[tile])
            )
            copies[-1].start()
        for copy in copies:
            copy.wait()

    inputs = [*pieces, weights] + ([] if total is None else [total])
    shape = (blocks, groups, parts, columns)
    scratch = [
        pltpu.VMEM((groups, blocks, parts, columns), jnp.bfloat16),
        pltpu.SemaphoreType.DMA((groups,)),
    ]
    return pl.pallas_call(
        finish if last else start,
        in_specs=[VMEM_SPEC] * len(inputs),
        out_specs=pl.BlockSpec(memory_space=pl.ANY) if last else VMEM_SPEC,
        out_shape=(
            jax.ShapeDtypeStruct(shape, jnp.bfloat16)
            if last
            else pltpu.VMEM((local, columns), jnp.float32)
        ),
        scratch_shapes=scratch if last else [],
        compiler_params=PARAMS,
        name="finish_pieces" if last else "add_pieces",
    )(*map(in_vmem, inputs))


def fast_device(tokens, proj_in, proj_out):
    ranks, _, near = (lax.axis_size(a) for a in (ROW, *COL))
    local = tokens.shape[0]
    group = proj_in.shape[1]
    items = group // ranks
    columns = proj_out.shape[1]
    rank, own = lax.axis_index(ROW), lax.axis_index(COL)
    order = [own, own ^ 1, own ^ near, own ^ near ^ 1]
    blocks = LANES // ranks
    swap = [(i, i ^ 1) for i in range(2)]
    packed = project_in(tokens, proj_in).reshape(ranks, items, local)
    values = lax.all_to_all(packed, ROW, split_axis=0, concat_axis=0, tiled=True)
    first = (rank * items).astype(jnp.int32).reshape(1)
    weights = fold_weights(proj_out, order, group, ranks, CHUNKS)
    found = []
    for c in range(CHUNKS):
        found.append(sequence_transform(values, first, group, c, CHUNKS))
    here, there, here_too, there_too = [], [], [], []
    for c in range(CHUNKS):
        back = lax.all_to_all(found[c], ROW, split_axis=0, concat_axis=0, tiled=True)
        here.append(back.reshape(-1, local))
        there.append(lax.ppermute(here[c], COL[0], swap))
        here_too.append(lax.ppermute(here[c], COL[1], swap))
    total = add_pieces([*here, *here_too], weights, 0, None, blocks, False)
    for c in range(CHUNKS):
        there_too.append(lax.ppermute(there[c], COL[1], swap))
    out = add_pieces([*there, *there_too], weights, 2 * group, total, blocks, True)
    return out.reshape(local, columns)


def solution(mesh):
    ranks, cols = mesh.devices.shape
    near = 2 if cols % 2 == 0 else 1
    inner = Mesh(mesh.devices.reshape(ranks, cols // near, near), (ROW, *COL))

    def program(tokens, proj_in, proj_out):
        local, group = tokens.shape[0] // ranks, proj_in.shape[1] // cols
        fits = (
            group == LANES
            and LANES % ranks == 0
            and ranks % 8 == 0
            and local % LANES == 0
            and near == 2
            and cols == 4
        )
        step = jax.shard_map(
            fast_device if fits else general_device,
            mesh=inner,
            in_specs=(P(ROW, None), P(None, COL), P(None, COL)),
            out_specs=P(ROW, COL),
            check_vma=False,
        )
        return step(tokens, proj_in, proj_out)

    return program
```
